32 devices in a mesh: kv: 8 (over z, x), tp: 4 (over y, core).
Axes of the slice: x: 2, y: 2, z: 4, core: 2. Of those that a mesh axis runs over, the one named last changes fastest.
Arguments:
- tokens: bfloat16 [32768, 2048], P('kv'), may hold values from -6 to 6
- w_query: bfloat16 [2048, 2048], P(None, 'tp'), may hold values from -0.125 to 0.125
- w_key: bfloat16 [2048, 2048], P(None, 'tp'), may hold values from -0.125 to 0.125
- w_value: bfloat16 [2048, 2048], P(None, 'tp'), may hold values from -0.125 to 0.125
- w_out: bfloat16 [2048, 2048], P('tp'), may hold values from -1 to 1, as said below
- query_gain: float32 [128], replicated, may hold values from 0.5 to 1.5
- key_gain: float32 [128], replicated, may hold values from 0.5 to 1.5
- out_gain: float32 [2048], replicated, may hold values from 0.5 to 1.5
- chosen: int32 [512, 8], P('kv'), may hold values from -1 to 511, as said below
Outputs:
- layer_out: bfloat16 [32768, 2048], P('kv', 'tp')
The draws below stay inside these ranges and needn't reach their ends.
Inputs may be any that keep to these rules, and one draw needn't show every extreme that they name: Row b of chosen lists min(8, b + 1) different key blocks, all at most b, with block b in the first slot, and -1 in the remaining slots. Split the blocks into groups of 64 consecutive blocks. The rows of one group other than the first name together at most 8 different blocks of the first group, and at most 2 different blocks of any other group but their own. Both bounds are reached. Entries of w_out have mean zero; the scale of a column grows smoothly with the feature index, by a factor of 8 from the first to the last feature.
All inputs are finite; a program needn't handle non-finite values.
Results may differ from the reference program's by a relative error of at most 0.025.
Values may be sent and summed in bfloat16 or wider, within the bound.
A program may use at most 256 MiB of HBM per device.

```python
import jax
import jax.numpy as jnp
from jax import lax

D = 2048
HEADS = 16
HEAD_DIM = 128
BLOCK = 64
CHOSEN = 8
HOT = 8
REACH = 2
QB_DEV = 64
QBLOCKS = 512
SEQ = 32768


def draw_w_out(key, part):
    rows = HEADS * HEAD_DIM
    base = jax.random.truncated_normal(key, -4.0, 4.0, (rows, D), jnp.float32)
    feature_pos = jnp.arange(D, dtype=jnp.float32) / D
    column_scale = jnp.exp2(3.0 * feature_pos - 1.5)
    return (base * column_scale[None, :] * rows ** (-0.5)).astype(jnp.bfloat16)


def draw_chosen(key, part):
    blocks_dev = QB_DEV
    owners = QBLOCKS // QB_DEV
    key_level, key_pool, key_pick = jax.random.split(key, 3)
    popularity = jax.random.randint(key_level, (QBLOCKS,), 0, 4)
    weight = 1 + popularity * popularity * popularity
    pool_jitter = jax.random.randint(key_pool, (owners, owners, blocks_dev), 0, 4096)
    positions = jnp.arange(blocks_dev, dtype=jnp.int32)
    pool_scores = pool_jitter * weight.reshape(owners, blocks_dev)[None] * blocks_dev + positions
    ranking = jnp.argsort(-pool_scores, axis=-1).astype(jnp.int32)
    first_pool = ranking[:, 0, :HOT]
    other_pool = ranking[:, :, :REACH]
    first_member = jnp.any(first_pool[:, :, None] == positions[None, None, :], axis=1)
    other_member = jnp.any(other_pool[:, :, :, None] == positions[None, None, None, :], axis=2)
    requester = jnp.arange(owners, dtype=jnp.int32)[:, None]
    owner_ids = jnp.arange(owners, dtype=jnp.int32)[None, :]
    member = jnp.where((owner_ids == 0)[:, :, None], first_member[:, None, :], other_member)
    member = member & (owner_ids < requester)[:, :, None]
    in_pool = member.reshape(owners, QBLOCKS)
    row_ids = jnp.arange(QBLOCKS, dtype=jnp.int32)
    device = row_ids // blocks_dev
    within = row_ids % blocks_dev
    forced_first = first_pool[device, within % HOT]
    previous = jnp.maximum(device - 1, 0)
    forced_second = other_pool[device, previous, within % REACH] + previous * blocks_dev
    columns = row_ids[None, :]
    local_earlier = (columns < row_ids[:, None]) & (columns >= (device * blocks_dev)[:, None])
    candidate = local_earlier | in_pool[device]
    candidate = candidate & jnp.logical_not((columns == forced_first[:, None]) & (device >= 1)[:, None])
    candidate = candidate & jnp.logical_not((columns == forced_second[:, None]) & (device >= 2)[:, None])
    jitter = jax.random.randint(key_pick, (QBLOCKS, QBLOCKS), 0, 4096)
    scores = jnp.where(candidate, jitter * weight[None, :] * QBLOCKS + columns, -1)
    values, picked = lax.top_k(scores, CHOSEN - 1)
    picked = jnp.where(values >= 0, picked, -1).astype(jnp.int32)
    trailing_one = jnp.concatenate([forced_first[:, None], picked[:, :CHOSEN - 2]], axis=1)
    trailing_two = jnp.concatenate([forced_first[:, None], forced_second[:, None], picked[:, :CHOSEN - 3]], axis=1)
    trailing = jnp.where((device >= 2)[:, None], trailing_two, jnp.where((device >= 1)[:, None], trailing_one, picked))
    return jnp.concatenate([row_ids[:, None], trailing], axis=1).astype(jnp.int32)


def shard_levels(key, dims, cuts, low, top_value):
    def one(position, parts):
        draws = jax.random.uniform(jax.random.fold_in(jax.random.fold_in(key, 6), position), (parts,), jnp.float32, low / len(cuts), top_value / len(cuts))
        return jnp.repeat(jnp.exp(draws), dims[position] // parts).reshape((-1,) + (1,) * (len(dims) - position - 1))

    gain = one(*cuts[0])
    for cut in cuts[1:]:
        gain = gain * one(*cut)
    return gain


def bell_draw(stream_key, shape, width, limit, cuts=(), kind=jnp.bfloat16):
    array = width * jax.random.normal(stream_key, shape, jnp.float32)
    if cuts:
        array = array * shard_levels(stream_key, shape, cuts, -0.22, 0.18)
    return jnp.clip(array, -limit, limit).astype(kind)


def setup_inputs(seed: int = 0) -> dict:
    streams_of = jax.random.split(jax.random.key(seed), 10)
    return {
        "tokens": bell_draw(streams_of[0], (SEQ, D), 1.0, 6.0, ((0, 8),)),
        "w_query": bell_draw(streams_of[1], (D, HEADS * HEAD_DIM), D ** -0.5, 0.125, ((1, 4),)),
        "w_key": bell_draw(streams_of[2], (D, HEADS * HEAD_DIM), D ** -0.5, 0.125, ((1, 4),)),
        "w_value": bell_draw(streams_of[3], (D, HEADS * HEAD_DIM), D ** -0.5, 0.125, ((1, 4),)),
        "w_out": draw_w_out(jax.random.fold_in(streams_of[9], 71), 0),
        "query_gain": jnp.clip(1.0 + 0.1 * jax.random.normal(streams_of[5], (HEAD_DIM,), jnp.float32), 0.5, 1.5),
        "key_gain": jnp.clip(1.0 + 0.1 * jax.random.normal(streams_of[6], (HEAD_DIM,), jnp.float32), 0.5, 1.5),
        "out_gain": jnp.clip(1.0 + 0.1 * jax.random.normal(streams_of[7], (D,), jnp.float32), 0.5, 1.5),
        "chosen": draw_chosen(jax.random.fold_in(streams_of[9], 71), 0),
    }


norm_eps = 1e-06

def head_norm(values, gain_row):
    factor = lax.rsqrt(lax.optimization_barrier(jnp.mean(values * values, axis=-1, keepdims=True)) + norm_eps)
    return (values * factor * gain_row).astype(jnp.bfloat16)

def project(tokens, weight):
    return jnp.dot(tokens, weight, preferred_element_type=jnp.float32).astype(jnp.bfloat16)

def reference(tokens, w_query, w_key, w_value, w_out, query_gain, key_gain, out_gain, chosen):
    length = tokens.shape[0]
    queries = project(tokens, w_query).reshape(length, HEADS, HEAD_DIM)
    queries = head_norm(queries.astype(jnp.float32), query_gain)
    key_rows = project(tokens, w_key).reshape(length, HEADS, HEAD_DIM)
    key_rows = head_norm(key_rows.astype(jnp.float32), key_gain)
    value_rows = project(tokens, w_value).reshape(length, HEADS, HEAD_DIM)
    key_blocks = key_rows.reshape(QBLOCKS, BLOCK, HEADS, HEAD_DIM)
    value_blocks = value_rows.reshape(QBLOCKS, BLOCK, HEADS, HEAD_DIM)
    groups = QBLOCKS // QB_DEV
    query_groups = queries.reshape(groups, QB_DEV, BLOCK, HEADS, HEAD_DIM)
    chosen_groups = chosen.reshape(groups, QB_DEV, CHOSEN)

    def one_group(group_item):
        query_part, picked_rows = group_item
        usable = picked_rows >= 0
        gather_at = jnp.where(usable, picked_rows, 0).astype(jnp.int32)
        key_sel = key_blocks[gather_at].astype(jnp.float32)
        value_sel = value_blocks[gather_at].astype(jnp.float32)
        logits = jnp.einsum('bqhd,bjkhd->bhqjk', query_part.astype(jnp.float32), key_sel) * HEAD_DIM ** (-0.5)
        logits = jnp.where(usable[:, None, None, :, None], logits, -jnp.inf)
        flattened = logits.reshape(QB_DEV, HEADS, BLOCK, CHOSEN * BLOCK)
        row_peak = lax.optimization_barrier(jnp.max(flattened, axis=-1, keepdims=True))
        weights = jnp.exp(flattened - row_peak)
        totals = lax.optimization_barrier(jnp.sum(weights, axis=-1))
        rounded = lax.optimization_barrier(weights.astype(jnp.bfloat16)).astype(jnp.float32)
        rounded = rounded.reshape(QB_DEV, HEADS, BLOCK, CHOSEN, BLOCK)
        combined = jnp.einsum('bhqjk,bjkhd->bqhd', rounded, value_sel)
        return (combined / jnp.transpose(totals, (0, 2, 1))[..., None]).astype(jnp.bfloat16)
    attended = lax.map(one_group, (query_groups, chosen_groups))
    attended = attended.reshape(length, HEADS * HEAD_DIM)
    combined = jnp.dot(attended, w_out, preferred_element_type=jnp.float32)
    factor = lax.rsqrt(lax.optimization_barrier(jnp.mean(combined * combined, axis=-1, keepdims=True)) + norm_eps)
    return (combined * factor * out_gain).astype(jnp.bfloat16)
```

```python
import functools

import jax
import jax.numpy as jnp
from jax import lax
from jax.experimental import pallas as pl
from jax.experimental.pallas import tpu as pltpu
from jax.sharding import PartitionSpec as P

HEAD_DIM = 128
BLOCK = 64
HOT = 8
REACH = 2
CHUNKS = 4
PROJECT_ROWS = 512
STEP_BLOCKS = 4


norm_eps = 1e-06
exp2_scale = HEAD_DIM ** (-0.5) * 1.4426950408889634


def project_kernel(normed, tokens_ref, *refs):
    count = len(normed)
    weight_refs, gain_ref, out_refs = refs[:count], refs[count], refs[count + 1:]
    rows = tokens_ref[...]
    for flag, weight_ref, out_ref in zip(normed, weight_refs, out_refs):
        product = jnp.dot(rows, weight_ref[...], preferred_element_type=jnp.float32)
        rounded = product.astype(jnp.bfloat16)
        if not flag:
            out_ref[...] = rounded
            continue
        for first in range(0, product.shape[1], HEAD_DIM):
            part = rounded[:, first:first + HEAD_DIM].astype(jnp.float32)
            mean = jnp.mean(part * part, axis=-1, keepdims=True)
            scaled = part * lax.rsqrt(mean + norm_eps) * gain_ref[...]
            out_ref[:, first:first + HEAD_DIM] = scaled.astype(jnp.bfloat16)


def project(tokens, weights, normed, gain):
    length, width = tokens.shape
    columns = weights[0].shape[1]
    rows = min(PROJECT_ROWS, length)
    whole = pl.BlockSpec((width, columns), lambda i: (0, 0))
    return pl.pallas_call(
        functools.partial(project_kernel, normed),
        grid=(length // rows,),
        in_specs=[pl.BlockSpec((rows, width), lambda i: (i, 0))]
        + [whole] * len(weights)
        + [pl.BlockSpec((1, HEAD_DIM), lambda i: (0, 0))],
        out_specs=[pl.BlockSpec((rows, columns), lambda i: (i, 0))] * len(weights),
        out_shape=[jax.ShapeDtypeStruct((length, columns), jnp.bfloat16)] * len(weights),
        compiler_params=pltpu.CompilerParams(vmem_limit_bytes=48 * 2**20),
        cost_estimate=pl.CostEstimate(
            flops=2 * length * width * columns * len(weights),
            bytes_accessed=2 * (length * width + len(weights) * columns * (length + width)),
            transcendentals=0,
        ),
    )(tokens, *weights, gain.reshape(1, HEAD_DIM))


def attend_kernel(first_block, slots, parts, at_ref, query_ref, bias_ref, w_out_ref, *refs):
    key_parts, value_parts = refs[:parts], refs[parts:2 * parts]
    out_ref, table_keys, table_values, attended, sems = refs[2 * parts:]
    heads = query_ref.shape[1] // HEAD_DIM
    step = pl.program_id(0)

    @pl.when(step == 0)
    def _():
        copies = []
        for group, table in ((key_parts, table_keys), (value_parts, table_values)):
            start = 0
            for part in group:
                size = part.shape[0]
                copies.append(
                    pltpu.make_async_copy(part, table.at[pl.ds(start, size)], sems.at[len(copies)])
                )
                start += size
        for copy in copies:
            copy.start()
        for copy in copies:
            copy.wait()

    for inner in range(STEP_BLOCKS):
        block = first_block + step * STEP_BLOCKS + inner
        starts = [pl.multiple_of(at_ref[block * slots + j] * BLOCK, BLOCK) for j in range(slots)]
        bias = bias_ref[inner]
        for head in range(heads):
            lanes = slice(head * HEAD_DIM, (head + 1) * HEAD_DIM)
            query = query_ref[inner * BLOCK:(inner + 1) * BLOCK, lanes]
            keys = jnp.concatenate([table_keys[pl.ds(s, BLOCK), lanes] for s in starts], axis=0)
            values = jnp.concatenate([table_values[pl.ds(s, BLOCK), lanes] for s in starts], axis=0)
            logits = lax.dot_general(
                query, keys, (((1,), (1,)), ((), ())), preferred_element_type=jnp.float32
            ) + bias
            peak = jnp.max(logits, axis=-1, keepdims=True)
            weights = jnp.exp2((logits - peak) * exp2_scale)
            total = jnp.sum(weights, axis=-1, keepdims=True)
            combined = jnp.dot(
                weights.astype(jnp.bfloat16), values, preferred_element_type=jnp.float32
            )
            attended[inner * BLOCK:(inner + 1) * BLOCK, lanes] = (combined / total).astype(
                jnp.bfloat16
            )
    rows = attended[...]
    features = out_ref.shape[2]
    for part in range(out_ref.shape[0]):
        out_ref[part] = jnp.dot(
            rows,
            w_out_ref[:, part * features:(part + 1) * features],
            preferred_element_type=jnp.float32,
        ).astype(jnp.bfloat16)


def attend(first_block, blocks, at, queries, bias, w_out, key_parts, value_parts, splits):
    slots = at.shape[0] // bias.shape[0]
    columns = queries.shape[1]
    features = w_out.shape[1] // splits
    rows = STEP_BLOCKS * BLOCK
    first_step = first_block // STEP_BLOCKS
    table_rows = sum(part.shape[0] for part in key_parts)
    parts = len(key_parts)
    length = blocks * BLOCK
    table_bytes = 4 * table_rows * columns
    return pl.pallas_call(
        functools.partial(attend_kernel, first_block, slots, parts),
        grid_spec=pltpu.PrefetchScalarGridSpec(
            num_scalar_prefetch=1,
            grid=(blocks // STEP_BLOCKS,),
            in_specs=[
                pl.BlockSpec((rows, columns), lambda i, at: (first_step + i, 0)),
                pl.BlockSpec((STEP_BLOCKS, 1, slots * BLOCK), lambda i, at: (first_step + i, 0, 0)),
                pl.BlockSpec(w_out.shape, lambda i, at: (0, 0)),
            ]
            + [pl.BlockSpec(memory_space=pl.ANY)] * (2 * parts),
            out_specs=pl.BlockSpec((splits, rows, features), lambda i, at: (0, i, 0)),
            scratch_shapes=[
                pltpu.VMEM((table_rows, columns), jnp.bfloat16),
                pltpu.VMEM((table_rows, columns), jnp.bfloat16),
                pltpu.VMEM((rows, columns), jnp.bfloat16),
                pltpu.SemaphoreType.DMA((2 * parts,)),
            ],
        ),
        out_shape=jax.ShapeDtypeStruct((splits, length, features), jnp.bfloat16),
        compiler_params=pltpu.CompilerParams(vmem_limit_bytes=48 * 2**20),
        cost_estimate=pl.CostEstimate(
            flops=2 * length * columns * (2 * slots * BLOCK + w_out.shape[1]),
            bytes_accessed=table_bytes + 2 * length * (columns + w_out.shape[1]),
            transcendentals=length * slots * BLOCK * columns // HEAD_DIM,
        ),
    )(at, queries, bias, w_out, *key_parts, *value_parts)


def body(tokens, w_query, w_key, w_value, w_out, query_gain, key_gain, out_gain, chosen):
    length, model_width = tokens.shape
    columns = w_query.shape[1]
    blocks_here = length // BLOCK
    slots_row = chosen.shape[1]
    devices = lax.axis_size("kv")
    splits = lax.axis_size("tp")
    position = lax.axis_index("kv")
    part_at = lax.axis_index("tp")

    usable = chosen >= 0
    flat_pick = jnp.where(usable, chosen, 0)
    owner_of = flat_pick // blocks_here
    inner_at = flat_pick % blocks_here
    all_blocks = jnp.arange(devices * blocks_here, dtype=jnp.int32)
    marked = jnp.where(usable, chosen, -1)
    wanted = jnp.any(marked[:, :, None] == all_blocks[None, None, :], axis=(0, 1)).reshape(
        devices, blocks_here
    )
    rank_of = jnp.cumsum(wanted.astype(jnp.int32), axis=1) - 1
    local_ids = jnp.arange(blocks_here, dtype=jnp.int32)
    places = wanted[:, :, None] & (
        rank_of[:, :, None] == jnp.arange(HOT, dtype=jnp.int32)[None, None, :]
    )
    requests = jnp.sum(jnp.where(places, local_ids[None, :, None], 0), axis=1).astype(jnp.int32)
    asked_for = lax.all_to_all(requests, "kv", split_axis=0, concat_axis=0, tiled=True)

    token_blocks = tokens.reshape(blocks_here, BLOCK, model_width)
    per_part = HOT // splits
    hot_part = None
    for target in range(1, devices):
        picks = lax.dynamic_slice_in_dim(asked_for[target], part_at * per_part, per_part, 0)
        moved = lax.ppermute(token_blocks[picks], "kv", [(0, target)])
        hot_part = moved if hot_part is None else jnp.where(position == target, moved, hot_part)
    hot_tokens = lax.all_gather(
        hot_part.reshape(per_part * BLOCK, model_width), "tp", axis=0, tiled=True
    )

    keys, values = project(tokens, (w_key, w_value), (True, False), key_gain)
    key_blocks = keys.reshape(blocks_here, BLOCK, columns)
    value_blocks = values.reshape(blocks_here, BLOCK, columns)
    reach_keys, reach_values = [], []
    for shift in range(1, devices - 1):
        pairs = [(owner, owner + shift) for owner in range(1, devices - shift)]
        row = jnp.minimum(position + shift, devices - 1)
        picks = lax.dynamic_slice(asked_for, (row, 0), (1, REACH))[0]
        reach_keys.append(lax.ppermute(key_blocks[picks], "kv", pairs))
        reach_values.append(lax.ppermute(value_blocks[picks], "kv", pairs))
    reach_keys = [part.reshape(REACH * BLOCK, columns) for part in reach_keys]
    reach_values = [part.reshape(REACH * BLOCK, columns) for part in reach_values]
    (queries,) = project(tokens, (w_query,), (True,), query_gain)
    hot_keys, hot_values = project(hot_tokens, (w_key, w_value), (True, False), key_gain)

    slot_rank = rank_of.reshape(-1)[flat_pick]
    remote_at = jnp.where(
        owner_of == 0, slot_rank, HOT + (position - owner_of - 1) * REACH + slot_rank
    )
    at = jnp.where(owner_of == position, inner_at, blocks_here + remote_at)
    at = jnp.where(usable, at, 0).astype(jnp.int32).reshape(-1)
    bias = jnp.where(usable, 0.0, -jnp.inf).astype(jnp.float32)
    bias = jnp.repeat(bias, BLOCK, axis=1).reshape(blocks_here, 1, slots_row * BLOCK)

    chunk = blocks_here // CHUNKS
    sums = []
    for index in range(CHUNKS):
        sent = attend(
            index * chunk, chunk, at, queries, bias, w_out,
            [keys, hot_keys] + reach_keys, [values, hot_values] + reach_values, splits,
        )
        sums.append(lax.psum_scatter(sent, "tp", scatter_dimension=0, tiled=False))
    squares = [jnp.sum(jnp.square(s.astype(jnp.float32)), axis=-1) for s in sums]
    squares = lax.psum(jnp.concatenate(squares), "tp")
    factor = lax.rsqrt(squares / model_width + norm_eps)
    features = model_width // splits
    gain_part = lax.dynamic_slice_in_dim(out_gain, part_at * features, features, 0)
    summed = jnp.concatenate(sums, axis=0).astype(jnp.float32)
    return (summed * factor[:, None] * gain_part[None, :]).astype(jnp.bfloat16)


def solution(mesh):
    in_specs = (
        P("kv", None),
        P(None, "tp"),
        P(None, "tp"),
        P(None, "tp"),
        P("tp", None),
        P(),
        P(),
        P(),
        P("kv", None),
    )
    out_specs = P("kv", "tp")
    return jax.shard_map(body, mesh=mesh, in_specs=in_specs, out_specs=out_specs, check_vma=False)
```

```python
import functools

import jax
import jax.numpy as jnp
from jax import lax
from jax.experimental import pallas as pl
from jax.experimental.pallas import tpu as pltpu
from jax.sharding import PartitionSpec as P

HEAD_DIM = 128
BLOCK = 64
HOT = 8
REACH = 2
FIRST_SHARE = 3
SHARES = 8
PROJECT_ROWS = 512
STEP_BLOCKS = 4


norm_eps = 1e-06
exp2_scale = HEAD_DIM ** (-0.5) * 1.4426950408889634


def project_kernel(normed, tokens_ref, *refs):
    count = len(normed)
    weight_refs, gain_ref, out_refs = refs[:count], refs[count], refs[count + 1:]
    rows = tokens_ref[...]
    for flag, weight_ref, out_ref in zip(normed, weight_refs, out_refs):
        product = jnp.dot(rows, weight_ref[...], preferred_element_type=jnp.float32)
        rounded = product.astype(jnp.bfloat16)
        if not flag:
            out_ref[...] = rounded
            continue
        for first in range(0, product.shape[1], HEAD_DIM):
            part = rounded[:, first:first + HEAD_DIM].astype(jnp.float32)
            mean = jnp.mean(part * part, axis=-1, keepdims=True)
            scaled = part * lax.rsqrt(mean + norm_eps) * gain_ref[...]
            out_ref[:, first:first + HEAD_DIM] = scaled.astype(jnp.bfloat16)


def project(tokens, weights, normed, gain):
    length, width = tokens.shape
    columns = weights[0].shape[1]
    rows = min(PROJECT_ROWS, length)
    whole = pl.BlockSpec((width, columns), lambda i: (0, 0))
    return pl.pallas_call(
        functools.partial(project_kernel, normed),
        grid=(length // rows,),
        in_specs=[pl.BlockSpec((rows, width), lambda i: (i, 0))]
        + [whole] * len(weights)
        + [pl.BlockSpec((1, HEAD_DIM), lambda i: (0, 0))],
        out_specs=[pl.BlockSpec((rows, columns), lambda i: (i, 0))] * len(weights),
        out_shape=[jax.ShapeDtypeStruct((length, columns), jnp.bfloat16)] * len(weights),
        compiler_params=pltpu.CompilerParams(vmem_limit_bytes=48 * 2**20),
        cost_estimate=pl.CostEstimate(
            flops=2 * length * width * columns * len(weights),
            bytes_accessed=2 * (length * width + len(weights) * columns * (length + width)),
            transcendentals=0,
        ),
    )(tokens, *weights, gain.reshape(1, HEAD_DIM))


def attend_kernel(first_block, slots, parts, at_ref, query_ref, bias_ref, w_out_ref, *refs):
    key_parts, value_parts = refs[:parts], refs[parts:2 * parts]
    out_ref, table_keys, table_values, attended, sems = refs[2 * parts:]
    heads = query_ref.shape[1] // HEAD_DIM
    step = pl.program_id(0)

    @pl.when(step == 0)
    def _():
        copies = []
        for group, table in ((key_parts, table_keys), (value_parts, table_values)):
            start = 0
            for part in group:
                size = part.shape[0]
                copies.append(
                    pltpu.make_async_copy(part, table.at[pl.ds(start, size)], sems.at[len(copies)])
                )
                start += size
        for copy in copies:
            copy.start()
        for copy in copies:
            copy.wait()

    for inner in range(STEP_BLOCKS):
        block = first_block + step * STEP_BLOCKS + inner
        starts = [pl.multiple_of(at_ref[block * slots + j] * BLOCK, BLOCK) for j in range(slots)]
        bias = bias_ref[inner]
        for head in range(heads):
            lanes = slice(head * HEAD_DIM, (head + 1) * HEAD_DIM)
            query = query_ref[inner * BLOCK:(inner + 1) * BLOCK, lanes]
            keys = jnp.concatenate([table_keys[pl.ds(s, BLOCK), lanes] for s in starts], axis=0)
            values = jnp.concatenate([table_values[pl.ds(s, BLOCK), lanes] for s in starts], axis=0)
            logits = lax.dot_general(
                query, keys, (((1,), (1,)), ((), ())), preferred_element_type=jnp.float32
            ) + bias
            weights = jnp.exp2(logits * exp2_scale)
            total = jnp.sum(weights, axis=-1, keepdims=True)
            combined = jnp.dot(
                weights.astype(jnp.bfloat16), values, preferred_element_type=jnp.float32
            )
            attended[inner * BLOCK:(inner + 1) * BLOCK, lanes] = (combined / total).astype(
                jnp.bfloat16
            )
    rows = attended[...]
    features = out_ref.shape[2]
    for part in range(out_ref.shape[0]):
        out_ref[part] = jnp.dot(
            rows,
            w_out_ref[:, part * features:(part + 1) * features],
            preferred_element_type=jnp.float32,
        ).astype(jnp.bfloat16)


def attend(first_block, blocks, at, queries, bias, w_out, key_parts, value_parts, splits):
    slots = at.shape[0] // bias.shape[0]
    columns = queries.shape[1]
    features = w_out.shape[1] // splits
    rows = STEP_BLOCKS * BLOCK
    first_step = first_block // STEP_BLOCKS
    table_rows = sum(part.shape[0] for part in key_parts)
    parts = len(key_parts)
    length = blocks * BLOCK
    table_bytes = 4 * table_rows * columns
    return pl.pallas_call(
        functools.partial(attend_kernel, first_block, slots, parts),
        grid_spec=pltpu.PrefetchScalarGridSpec(
            num_scalar_prefetch=1,
            grid=(blocks // STEP_BLOCKS,),
            in_specs=[
                pl.BlockSpec((rows, columns), lambda i, at: (first_step + i, 0)),
                pl.BlockSpec((STEP_BLOCKS, 1, slots * BLOCK), lambda i, at: (first_step + i, 0, 0)),
                pl.BlockSpec(w_out.shape, lambda i, at: (0, 0)),
            ]
            + [pl.BlockSpec(memory_space=pl.ANY)] * (2 * parts),
            out_specs=pl.BlockSpec((splits, rows, features), lambda i, at: (0, i, 0)),
            scratch_shapes=[
                pltpu.VMEM((table_rows, columns), jnp.bfloat16),
                pltpu.VMEM((table_rows, columns), jnp.bfloat16),
                pltpu.VMEM((rows, columns), jnp.bfloat16),
                pltpu.SemaphoreType.DMA((2 * parts,)),
            ],
        ),
        out_shape=jax.ShapeDtypeStruct((splits, length, features), jnp.bfloat16),
        compiler_params=pltpu.CompilerParams(vmem_limit_bytes=48 * 2**20),
        cost_estimate=pl.CostEstimate(
            flops=2 * length * columns * (2 * slots * BLOCK + w_out.shape[1]),
            bytes_accessed=table_bytes + 2 * length * (columns + w_out.shape[1]),
            transcendentals=length * slots * BLOCK * columns // HEAD_DIM,
        ),
    )(at, queries, bias, w_out, *key_parts, *value_parts)


def pick_blocks(rows, picks):
    return jnp.concatenate(
        [
            lax.dynamic_slice_in_dim(rows, picks[i] * BLOCK, BLOCK, 0)
            for i in range(picks.shape[0])
        ],
        axis=0,
    )


def body(tokens, w_query, w_key, w_value, w_out, query_gain, key_gain, out_gain, chosen):
    length, model_width = tokens.shape
    columns = w_query.shape[1]
    blocks_here = length // BLOCK
    slots_row = chosen.shape[1]
    devices = lax.axis_size("kv")
    splits = lax.axis_size("tp")
    position = lax.axis_index("kv")
    part_at = lax.axis_index("tp")

    usable = chosen >= 0
    flat_pick = jnp.where(usable, chosen, 0)
    owner_of = flat_pick // blocks_here
    inner_at = flat_pick % blocks_here
    all_blocks = jnp.arange(devices * blocks_here, dtype=jnp.int32)
    marked = jnp.where(usable, chosen, -1)
    wanted = jnp.any(marked[:, :, None] == all_blocks[None, None, :], axis=(0, 1)).reshape(
        devices, blocks_here
    )
    rank_of = jnp.cumsum(wanted.astype(jnp.int32), axis=1) - 1
    local_ids = jnp.arange(blocks_here, dtype=jnp.int32)
    places = wanted[:, :, None] & (
        rank_of[:, :, None] == jnp.arange(HOT, dtype=jnp.int32)[None, None, :]
    )
    requests = jnp.sum(jnp.where(places, local_ids[None, :, None], 0), axis=1).astype(jnp.int32)
    asked_for = lax.all_to_all(requests, "kv", split_axis=0, concat_axis=0, tiled=True)

    per_part = HOT // splits
    arrivals = []
    for target in range(1, devices):
        picks = lax.dynamic_slice_in_dim(asked_for[target], part_at * per_part, per_part, 0)
        arrivals.append(lax.ppermute(pick_blocks(tokens, picks), "kv", [(0, target)]))

    keys, values = project(tokens, (w_key, w_value), (True, False), key_gain)
    *arrivals, keys, values = lax.optimization_barrier((*arrivals, keys, values))
    hot_part = arrivals[0]
    for target in range(2, devices):
        hot_part = jnp.where(position == target, arrivals[target - 1], hot_part)
    hot_tokens = lax.all_gather(hot_part, "tp", axis=0, tiled=True)
    reach_keys, reach_values = [], []
    for shift in range(1, devices - 1):
        pairs = [(owner, owner + shift) for owner in range(1, devices - shift)]
        row = jnp.minimum(position + shift, devices - 1)
        picks = lax.dynamic_slice(asked_for, (row, 0), (1, REACH))[0]
        reach_keys.append(lax.ppermute(pick_blocks(keys, picks), "kv", pairs))
        reach_values.append(lax.ppermute(pick_blocks(values, picks), "kv", pairs))
    (queries,) = project(tokens, (w_query,), (True,), query_gain)
    hot_keys, hot_values = project(hot_tokens, (w_key, w_value), (True, False), key_gain)

    slot_rank = rank_of.reshape(-1)[flat_pick]
    remote_at = jnp.where(
        owner_of == 0, slot_rank, HOT + (position - owner_of - 1) * REACH + slot_rank
    )
    at = jnp.where(owner_of == position, inner_at, blocks_here + remote_at)
    at = jnp.where(usable, at, 0).astype(jnp.int32).reshape(-1)
    bias = jnp.where(usable, 0.0, -jnp.inf).astype(jnp.float32)
    bias = jnp.repeat(bias, BLOCK, axis=1).reshape(blocks_here, 1, slots_row * BLOCK)

    first_size = blocks_here * FIRST_SHARE // SHARES // STEP_BLOCKS * STEP_BLOCKS
    sums = []
    for first, size in ((0, first_size), (first_size, blocks_here - first_size)):
        sent = attend(
            first, size, at, queries, bias, w_out,
            [keys, hot_keys] + reach_keys, [values, hot_values] + reach_values, splits,
        )
        sums.append(lax.psum_scatter(sent, "tp", scatter_dimension=0, tiled=False))
    squares = [jnp.sum(jnp.square(s.astype(jnp.float32)), axis=-1) for s in sums]
    squares = lax.psum(jnp.concatenate(squares), "tp")
    factor = lax.rsqrt(squares / model_width + norm_eps)
    features = model_width // splits
    gain_part = lax.dynamic_slice_in_dim(out_gain, part_at * features, features, 0)
    summed = jnp.concatenate(sums, axis=0).astype(jnp.float32)
    return (summed * factor[:, None] * gain_part[None, :]).astype(jnp.bfloat16)


def solution(mesh):
    in_specs = (
        P("kv", None),
        P(None, "tp"),
        P(None, "tp"),
        P(None, "tp"),
        P("tp", None),
        P(),
        P(),
        P(),
        P("kv", None),
    )
    out_specs = P("kv", "tp")
    return jax.shard_map(body, mesh=mesh, in_specs=in_specs, out_specs=out_specs, check_vma=False)
```
